256 devices in a mesh: ep: 16 (over y, x), tp: 16 (over z, core).
Axes of the slice: x: 4, y: 4, z: 8, core: 2. Of those that a mesh axis runs over, the one named last changes fastest.
Arguments:
- tokens: bfloat16 [1024, 2048], P('ep', 'tp'), may hold values from -64 to 64
- mixer_gain: float32 [2048], replicated, may hold values from 0.1 to 1.9
- expert_gain: float32 [2048], replicated, may hold values from 0.1 to 1.9
- query_weight: bfloat16 [2048, 1024], P(None, 'tp'), may hold values from -0.125 to 0.125
- key_weight: bfloat16 [2048, 1024], P(None, 'tp'), may hold values from -0.125 to 0.125
- value_weight: bfloat16 [2048, 4, 256], P(None, None, 'tp'), may hold values from -0.125 to 0.125
- outgate_weight: bfloat16 [2048, 4, 256], P(None, None, 'tp'), may hold values from -0.125 to 0.125
- ingate_weight: bfloat16 [2048, 4], replicated, may hold values from -0.125 to 0.125
- forget_weight: bfloat16 [2048, 4], replicated, may hold values from -0.125 to 0.125
- forget_bias: float32 [4], replicated, may hold values from -1 to 4
- mixout_weight: bfloat16 [1024, 2048], replicated, may hold values from -0.1875 to 0.1875
- memory_state: float32 [1024, 4, 256, 256], P('ep', None, 'tp'), may hold values from -0.6 to 0.6
- norm_state: float32 [1024, 4, 256], P('ep'), may hold values from -0.6 to 0.6
- max_state: float32 [1024, 4], P('ep'), may hold values from -4 to 4
- expert_gate: bfloat16 [256, 2048, 256], P(('ep', 'tp')), may hold values from -0.125 to 0.125
- expert_up: bfloat16 [256, 2048, 256], P(('ep', 'tp')), may hold values from -0.125 to 0.125
- expert_down: bfloat16 [256, 256, 2048], P(('ep', 'tp')), may hold values from -0.1875 to 0.1875
- routes: int32 [1024, 2], P('ep'), may hold values from 0 to 63, all different within a row; in each aligned block of 64 rows (0 to 63, 64 to 127, ...) at most 4 rows name the same one
- route_weights: float32 [1024, 2], P('ep'), may hold values from 0.1 to 1
Outputs:
- mixed_out: bfloat16 [1024, 2048], P('ep', 'tp')
- memory_next: float32 [1024, 4, 256, 256], P('ep', None, 'tp')
- norm_next: float32 [1024, 4, 256], P('ep')
- max_next: float32 [1024, 4], P('ep')
The draws below stay inside these ranges and needn't reach their ends.
Inputs may be any that keep to these rules, and one draw needn't show every extreme that they name: `routes`: each row names 2 different experts; in the rows of one index of ep (aligned blocks of 64 rows) no expert is named by more than 4 rows, a bound that some block reaches.
All inputs are finite; a program needn't handle non-finite values.
Results may differ from the reference program's by a relative error of at most 0.0079.
Values may be sent and summed in bfloat16 or wider, within the bound.
A program may use at most 64 MiB of HBM per device.

```python
import math
import jax
import jax.numpy as jnp
import numpy as np
from jax import lax

D = 2048
HEADS = 4
HEAD_DIM = 256
FF = 1024
FF_SPLIT = 4
TOPK = 2
SEQS = 64
BATCH = 1024
EXPERTS = 64
CAP = 4
N_EP = 16


def draw_tokens(key, part):
    key_base, key_rows = jax.random.split(key, 2)
    column_scale = jnp.exp(jnp.log(4.0) * (jnp.arange(D, dtype=jnp.float32) / D - 0.5))
    base_draw = jnp.clip(jax.random.normal(key_base, (BATCH, D), jnp.float32), -6.0, 6.0)
    row_scale = jnp.exp(jax.random.uniform(key_rows, (BATCH, 1), jnp.float32, jnp.log(0.5), jnp.log(5.0)))
    return (base_draw * column_scale * row_scale).astype(jnp.bfloat16)


def level_of(own_key, shape, cuts, least, high):
    level, own = 1.0, jax.random.fold_in(own_key, 6)
    for dim, blocks in cuts:
        draws = jnp.exp(jax.random.uniform(jax.random.fold_in(own, dim), (blocks,), jnp.float32, least / len(cuts), high / len(cuts)))
        level = level * jnp.repeat(draws, shape[dim] // blocks).reshape([-1 if axis == dim else 1 for axis in range(len(shape))])
    return level


def deal_out(key, own, number, rows, amount, top, limit, lean):
    order = jax.random.permutation(key, amount)
    crowded, common = portions_of(amount, rows * top, limit, lean, True), portions_of(amount, rows * top, limit, lean, False)
    places = jnp.arange(amount)

    def named(lengths, turn):
        used = int((lengths > 0).sum())
        fixed = max(1, used // 4)
        moved = fixed + (places - fixed + turn * (used - fixed)) % max(1, amount - fixed)
        return jnp.zeros((amount,), jnp.int32).at[order[jnp.where(places < fixed, places, moved)]].set(jnp.asarray(lengths, jnp.int32))

    lengths = jnp.where(number % 4 == 0, named(crowded, number // 4), named(common, number - number // 4 - 1))
    mixed = jax.random.permutation(jax.random.fold_in(own, 3), amount)
    giver, sink = mixed[0:amount // 2 * 2:2], mixed[1:amount // 2 * 2:2]
    slack = jnp.minimum(lengths[giver] - 1, limit - lengths[sink]) // 2
    slack = jnp.where((giver == order[0]) | (sink == order[0]) | (lengths[sink] == 0), 0, jnp.maximum(slack, 0))
    moved = jax.random.randint(jax.random.fold_in(own, 4), (amount // 2,), 0, 1 << 20) % (slack + 1)
    lengths = lengths.at[giver].add(-moved).at[sink].add(moved)
    items = jnp.searchsorted(jnp.cumsum(lengths), jnp.arange(rows * top), side="right").astype(jnp.int32)
    listing = items.reshape(top, rows).T
    listing = listing[jax.random.permutation(jax.random.fold_in(own, 1), rows)]
    turn = jax.random.randint(jax.random.fold_in(own, 2), (rows, 1), 0, top)
    return jnp.take_along_axis(listing, (jnp.arange(top)[None, :] + turn) % top, axis=1)


def portions_of(number_of, total, most, slope, full):
    loads = [(1 << 20) // math.isqrt(standing ** slope) + 1 for standing in range(1, number_of + 1)]
    largest = most if full else min(most, max(-(-total // number_of), total * loads[0] // sum(loads)))
    least = 1 if total - largest >= number_of - 1 else 0
    counts, spare = [largest] + [least] * (number_of - 1), total - largest - least * (number_of - 1)
    while spare > 0:
        movable = [i for i in range(1, number_of) if counts[i] < largest] or [i for i in range(1, number_of) if counts[i] < most]
        whole, remaining = sum([loads[i] for i in movable]), spare
        for i in movable:
            addition = min(most - counts[i], max(1, remaining * loads[i] // whole), spare)
            counts[i] = counts[i] + addition
            spare = spare - addition
    return np.array(counts)


def gaussian(rng, shape, scale, bound, cuts=(), held_as=jnp.bfloat16):
    loudness = level_of(rng, shape, cuts, -0.22, 0.18) if cuts else 1.0
    array = jax.random.normal(rng, shape, jnp.float32) * scale * loudness
    return jnp.minimum(jnp.maximum(array, -bound), bound).astype(held_as)


def setup_inputs(seed: int = 0) -> dict:
    seeds = jax.random.split(jax.random.key(seed), 20)
    tokens = draw_tokens(jax.random.fold_in(seeds[19], 71), 0)
    mixer_gain = jnp.clip(1.0 + 0.18 * jax.random.normal(seeds[1], (D,), jnp.float32), 0.1, 1.9)
    expert_gain = jnp.clip(1.0 + 0.18 * jax.random.normal(seeds[2], (D,), jnp.float32), 0.1, 1.9)
    query_weight = gaussian(seeds[3], (D, HEADS * HEAD_DIM), D ** -0.5, 0.125, ((1, 16),))
    key_weight = gaussian(seeds[4], (D, HEADS * HEAD_DIM), D ** -0.5, 0.125, ((1, 16),))
    value_weight = gaussian(seeds[5], (D, HEADS, HEAD_DIM), D ** -0.5, 0.125, ((2, 16),))
    outgate_weight = gaussian(seeds[6], (D, HEADS, HEAD_DIM), D ** -0.5, 0.125, ((2, 16),))
    ingate_weight = gaussian(seeds[7], (D, HEADS), D ** -0.5, 0.125)
    forget_weight = gaussian(seeds[8], (D, HEADS), D ** -0.5, 0.125)
    forget_bias = jnp.clip(jax.random.uniform(seeds[9], (HEADS,), jnp.float32, -1.0, 4.0), -1.0, 4.0)
    mixout_weight = gaussian(seeds[10], (HEADS * HEAD_DIM, D), (HEADS * HEAD_DIM) ** -0.5, 0.1875)
    memory_state = gaussian(seeds[11], (BATCH, HEADS, HEAD_DIM, HEAD_DIM), 0.1, 0.6, ((0, 16), (2, 16)), jnp.float32)
    norm_state = gaussian(seeds[12], (BATCH, HEADS, HEAD_DIM), 0.1, 0.6, ((0, 16),), jnp.float32)
    max_state = gaussian(seeds[13], (BATCH, HEADS), 1.0, 4.0, ((0, 16),), jnp.float32)
    expert_gate = gaussian(seeds[14], (EXPERTS * FF_SPLIT, D, FF // FF_SPLIT), D ** -0.5, 0.125, ((0, 256),))
    expert_up = gaussian(seeds[15], (EXPERTS * FF_SPLIT, D, FF // FF_SPLIT), D ** -0.5, 0.125, ((0, 256),))
    expert_down = gaussian(seeds[16], (EXPERTS * FF_SPLIT, FF // FF_SPLIT, D), FF ** -0.5, 0.1875, ((0, 256),))
    routes_keys = jax.random.split(jax.random.fold_in(seeds[17], 1), BATCH // SEQS)
    routes_turns = jax.random.permutation(jax.random.fold_in(seeds[17], 3), BATCH // SEQS)
    routes = jax.vmap(lambda own, number: deal_out(jax.random.fold_in(seeds[17], 2), own, number, SEQS, EXPERTS, TOPK, CAP, 2))(routes_keys, routes_turns).reshape((BATCH, TOPK))
    route_weights = jnp.clip(jnp.exp(math.log(1.0) - 2.3025851 * jax.random.uniform(seeds[18], (BATCH, TOPK), jnp.float32) ** level_of(seeds[18], (BATCH, TOPK), ((0, 16),), -0.2, 0.2)), 0.1, 1.0)
    return dict(tokens=tokens, mixer_gain=mixer_gain, expert_gain=expert_gain, query_weight=query_weight, key_weight=key_weight, value_weight=value_weight, outgate_weight=outgate_weight, ingate_weight=ingate_weight, forget_weight=forget_weight, forget_bias=forget_bias, mixout_weight=mixout_weight, memory_state=memory_state, norm_state=norm_state, max_state=max_state, expert_gate=expert_gate, expert_up=expert_up, expert_down=expert_down, routes=routes, route_weights=route_weights)


eps = 1e-06

def run_expert(packed):
    row_block, gate_blocks, up_blocks, down_blocks = packed
    block_count, width, block_units = gate_blocks.shape
    gate_mat = jnp.moveaxis(gate_blocks, 0, 1).reshape(width, block_count * block_units)
    up_mat = jnp.moveaxis(up_blocks, 0, 1).reshape(width, block_count * block_units)
    down_mat = down_blocks.reshape(block_count * block_units, down_blocks.shape[2])
    gate_part = jnp.dot(row_block, gate_mat, preferred_element_type=jnp.float32)
    up_part = jnp.dot(row_block, up_mat, preferred_element_type=jnp.float32)
    hidden = (jax.nn.silu(gate_part) * up_part).astype(jnp.bfloat16)
    return jnp.dot(hidden, down_mat, preferred_element_type=jnp.float32).astype(jnp.bfloat16)

def reference(tokens, mixer_gain, expert_gain, query_weight, key_weight, value_weight, outgate_weight, ingate_weight, forget_weight, forget_bias, mixout_weight, memory_state, norm_state, max_state, expert_gate, expert_up, expert_down, routes, route_weights):
    row_count = tokens.shape[0]
    token_float = tokens.astype(jnp.float32)
    inverse = lax.rsqrt(lax.optimization_barrier(jnp.mean(token_float * token_float, axis=1, keepdims=True)) + eps)
    scaled = (token_float * mixer_gain).astype(jnp.bfloat16)
    query_full = (inverse * jnp.dot(scaled, query_weight, preferred_element_type=jnp.float32)).reshape(row_count, HEADS, HEAD_DIM)
    key_full = (inverse * jnp.dot(scaled, key_weight, preferred_element_type=jnp.float32) * HEAD_DIM ** (-0.5)).reshape(row_count, HEADS, HEAD_DIM)
    values = (inverse * jnp.dot(scaled, value_weight.reshape(D, HEADS * HEAD_DIM), preferred_element_type=jnp.float32)).reshape(row_count, HEADS, HEAD_DIM)
    outgate = (inverse * jnp.dot(scaled, outgate_weight.reshape(D, HEADS * HEAD_DIM), preferred_element_type=jnp.float32)).reshape(row_count, HEADS, HEAD_DIM)
    ingate = inverse * jnp.dot(scaled, ingate_weight, preferred_element_type=jnp.float32)
    logforget = jax.nn.log_sigmoid(inverse * jnp.dot(scaled, forget_weight, preferred_element_type=jnp.float32) + forget_bias)
    max_next = jnp.maximum(logforget + max_state, ingate)
    decay_rate = jnp.exp(logforget + max_state - max_next)
    inflow = jnp.exp(ingate - max_next)
    memory_next = decay_rate[:, :, None, None] * memory_state + inflow[:, :, None, None] * values[:, :, :, None] * key_full[:, :, None, :]
    norm_next = decay_rate[:, :, None] * norm_state + inflow[:, :, None] * key_full
    numerator = jnp.einsum('bhvk,bhk->bhv', memory_next, query_full, precision=lax.Precision.HIGHEST)
    denominator = jnp.maximum(jnp.abs(lax.optimization_barrier(jnp.sum(norm_next * query_full, axis=2))), jnp.exp(-max_next))
    gated_heads = (jax.nn.sigmoid(outgate) * (numerator / denominator[:, :, None])).astype(jnp.bfloat16)
    middle = (token_float + jnp.dot(gated_heads.reshape(row_count, HEADS * HEAD_DIM), mixout_weight, preferred_element_type=jnp.float32)).astype(jnp.bfloat16)
    middle_float = middle.astype(jnp.float32)
    inverse_two = lax.rsqrt(lax.optimization_barrier(jnp.mean(middle_float * middle_float, axis=1, keepdims=True)) + eps)
    normed = (middle_float * inverse_two * expert_gain).astype(jnp.bfloat16)
    grouped = routes.reshape(N_EP, SEQS * TOPK)
    onehot = (grouped[:, :, None] == jnp.arange(EXPERTS, dtype=jnp.int32)[None, None, :]).astype(jnp.int32)
    slot_rank = lax.optimization_barrier(jnp.sum(onehot * (jnp.cumsum(onehot, axis=1) - 1), axis=2))
    row_index = (jnp.arange(N_EP, dtype=jnp.int32)[:, None] * CAP + slot_rank).reshape(-1).astype(jnp.int32)
    expert_index = grouped.reshape(-1).astype(jnp.int32)
    token_index = (jnp.arange(row_count * TOPK, dtype=jnp.int32) // TOPK).astype(jnp.int32)
    buffer = jnp.zeros((EXPERTS, N_EP * CAP, D), jnp.bfloat16).at[expert_index, row_index].set(normed[token_index])
    gate_blocks = expert_gate.reshape(EXPERTS, FF_SPLIT, D, FF // FF_SPLIT)
    up_blocks = expert_up.reshape(EXPERTS, FF_SPLIT, D, FF // FF_SPLIT)
    down_blocks = expert_down.reshape(EXPERTS, FF_SPLIT, FF // FF_SPLIT, D)
    results = lax.map(run_expert, (buffer, gate_blocks, up_blocks, down_blocks))
    picked = results[expert_index, row_index].astype(jnp.float32).reshape(row_count, TOPK, D)
    shares = route_weights / lax.optimization_barrier(jnp.sum(route_weights, axis=1, keepdims=True))
    mixed_out = (middle_float + lax.optimization_barrier(jnp.sum(shares[:, :, None] * picked, axis=1))).astype(jnp.bfloat16)
    return (mixed_out, memory_next, norm_next, max_next)
```

```python
import jax
import jax.numpy as jnp
from jax import lax
from jax.experimental import pallas as pl
from jax.experimental.pallas import tpu as pltpu
from jax.sharding import PartitionSpec as P

MESH = pl.DeviceIdType.MESH
F32, BF16 = jnp.float32, jnp.bfloat16
eps = 1e-06
ROWS, WIDTH, NTP, NEP, HEADS, HDIM, CAP, SPLIT = 64, 2048, 16, 16, 4, 256, 4, 4


def nt(a, b):
    return lax.dot_general(a, b, (((1,), (1,)), ((), ())), preferred_element_type=F32)


def nn(a, b):
    return jnp.dot(a, b, preferred_element_type=F32)


def iota(shape, dim):
    return lax.broadcasted_iota(jnp.int32, shape, dim)


def body(
    tok, gain_m, gain_e, qw, kw, vw, ow, igw, fgw, bias, mixout, mem, norm, mstate, egate, eup, edown, rt, rw,
    mixed, kfull, vout, dec_out, inf_out, max_out,
    xg, wall, igs, fgs, wgf, gms, ges, memv, memb, normv, mixw, egv, euv, edv, sm, mss, rts, rws, perm, perm2,
    comb, pbt, pbf, nso, scaled, qkb, pb, gb, mid, nst, sbuf, rbuf, dbuf, zbuf, obuf, fbuf,
    lsem, ssem, rsem,
):
    ep, tp = lax.axis_index("ep"), lax.axis_index("tp")
    group, block = tp // SPLIT, tp % SPLIT

    def local(i, src, dst):
        return pltpu.make_async_copy(src, dst, lsem.at[i])

    loads = [
        local(0, tok, xg.at[tp]),
        local(1, rt, rts), local(2, rw, rws), local(3, mstate, mss),
        local(4, igw, igs), local(5, fgw, fgs), local(6, gain_m, gms), local(7, gain_e, ges),
        local(8, qw, wall.at[0:64]), local(9, kw, wall.at[64:128]),
        local(10, vw, wall.at[128:192]), local(11, ow, wall.at[192:256]),
        local(12, norm, normv), local(13, mem, memv),
    ]
    loads += [local(14 + h, mixout.at[h], mixw.at[:, h]) for h in range(HEADS)]
    loads += [local(18, egate, egv), local(19, eup, euv), local(20, edown, edv)]
    for c in loads:
        c.start()

    barrier = pltpu.get_barrier_semaphore()

    def greet(d, _):
        pl.semaphore_signal(barrier, inc=1, device_id=(ep, lax.rem(tp + d, NTP)), device_id_type=MESH)
        pl.semaphore_signal(barrier, inc=1, device_id=(lax.rem(ep + d, NEP), tp), device_id_type=MESH)
        return 0

    lax.fori_loop(1, 16, greet, 0)

    i, j = iota((256, 256), 0), iota((256, 256), 1)
    perm[...] = (j == (((i >> 2) & 15) << 4) + ((i >> 6) << 2) + (i & 3)).astype(F32).astype(BF16)
    i, c = iota((256, 1024), 0), iota((256, 1024), 1)
    perm2[...] = (
        (((c >> 8) == ((i >> 2) & 3)) & ((c & 63) == ((i >> 4) << 2) + (i & 3))).astype(F32).astype(BF16)
    )

    pl.semaphore_wait(barrier, 30)

    def over_tp(phase, src, dst, peer_of_src):
        def copy(d):
            peer = lax.rem(tp + d, NTP)
            return pltpu.make_async_remote_copy(
                src_ref=src(peer), dst_ref=dst(tp), send_sem=ssem.at[phase, peer], recv_sem=rsem.at[phase, tp],
                device_id=(ep, peer), device_id_type=MESH)
        return copy

    def over_ep(phase, src, dst):
        def copy(d):
            peer = lax.rem(ep + d, NEP)
            return pltpu.make_async_remote_copy(
                src_ref=src(peer), dst_ref=dst(ep), send_sem=ssem.at[phase, peer], recv_sem=rsem.at[phase, ep],
                device_id=(peer, tp), device_id_type=MESH)
        return copy

    def start_all(copy):
        def step(d, _):
            copy(d).start()
            return 0
        lax.fori_loop(1, 16, step, 0)

    def sent_all(copy):
        def step(d, _):
            copy(d).wait_send()
            return 0
        lax.fori_loop(1, 16, step, 0)

    def arrived(phase, dst, me, axis_pos):
        def step(d, _):
            peer = lax.rem(me + d, 16)
            pltpu.make_async_remote_copy(
                src_ref=dst(peer), dst_ref=dst(peer), send_sem=ssem.at[phase, peer], recv_sem=rsem.at[phase, peer],
                device_id=axis_pos(peer), device_id_type=MESH).wait_recv()
            return 0
        lax.fori_loop(1, 16, step, 0)

    def tp_pos(peer):
        return (ep, peer)

    def ep_pos(peer):
        return (peer, tp)

    send_tok = over_tp(0, lambda p: xg.at[tp], lambda me: xg.at[me], None)
    send_qk = over_tp(1, lambda p: qkb.at[tp], lambda me: qkb.at[me], None)
    send_pb = over_tp(2, lambda p: pb.at[tp], lambda me: pb.at[me], None)
    send_g = over_tp(3, lambda p: gb.at[tp], lambda me: gb.at[me], None)
    send_rows = over_ep(4, lambda p: sbuf.at[p], lambda me: rbuf.at[me])
    send_z = over_tp(5, lambda p: dbuf.at[p], lambda me: zbuf.at[me], None)
    send_f = over_ep(6, lambda p: obuf.at[p], lambda me: fbuf.at[me])

    loads[0].wait()
    start_all(send_tok)

    for c in loads[1:8]:
        c.wait()
    sm[...] = jnp.zeros((128, 128), F32)
    sm[0:4, 0:64] = mss[...]
    sm[4:6, 0:64] = rws[...]
    sm[6:8, 0:64] = rts[...].astype(F32)
    cols = jnp.transpose(sm[...])[0:ROWS]
    w0, w1, r0, r1 = cols[:, 4:5], cols[:, 5:6], cols[:, 6:7], cols[:, 7:8]
    total = w0 + w1
    before = (iota((ROWS, ROWS), 1) < iota((ROWS, ROWS), 0)).astype(F32).astype(BF16)
    lane = iota((ROWS, 256), 1)
    slot_of = (lane & 3).astype(F32)
    expert = (lane >> 2).astype(F32)
    zero = jnp.zeros((ROWS, 256), F32)
    named0, named1 = r0 == expert, r1 == expert
    hit = jnp.where(named0 | named1, 1.0, zero)
    share = jnp.where(named0, w0 / total, zero) + jnp.where(named1, w1 / total, zero)
    share = jnp.where(nn(before, hit.astype(BF16)) == slot_of, share, zero)
    high = share.astype(BF16)
    comb[0:64] = high
    comb[64:128] = (share - high.astype(F32)).astype(BF16)
    expert = ((lane >> 4) * SPLIT + group).astype(F32)
    hit = jnp.where((r0 == expert) | (r1 == expert), 1.0, zero)
    pick = jnp.where(nn(before, hit.astype(BF16)) == slot_of, hit, zero)
    quarter = (lane >> 2) & 3
    for q in range(4):
        pbf[q * 64 : (q + 1) * 64] = jnp.where(quarter == q, pick, zero)
    pbt[...] = jnp.transpose(pbf[...]).astype(BF16)

    wgf[...] = jnp.zeros((16, WIDTH), F32)
    wgf[0:4] = igs[...].astype(F32)
    wgf[4:8] = fgs[...].astype(F32)
    wall[256:384] = jnp.zeros((128, WIDTH), BF16)
    wall[256:272] = wgf[...].astype(BF16)
    for c in loads[8:14]:
        c.wait()

    def narrow(k, _):
        at = pl.multiple_of(k * 8, 8)
        to = pl.multiple_of(k * 128, 128)
        for h in range(HEADS):
            memb[h, pl.ds(to, 128), :] = memv[pl.ds(at, 8), h].reshape(128, HDIM).astype(BF16)
        return 0

    lax.fori_loop(0, 8, narrow, 0)

    place = jnp.full((ROWS, 128), tp, jnp.int32)
    chosen = jnp.zeros((ROWS, 128), F32)
    for half in range(8):
        piece = normv[:, half // 2, (half % 2) * 128 : (half % 2 + 1) * 128]
        chosen = jnp.where(place >> 1 == half, piece, chosen)
    nso[...] = jnp.where((place & 1) == 1, pltpu.roll(chosen, 64, 1), chosen)

    arrived(0, lambda p: xg.at[p], tp, tp_pos)
    square = jnp.zeros((ROWS, 128), F32)
    for b in range(NTP):
        x = xg[b].astype(F32)
        square += x * x
        scaled[:, b * 128 : (b + 1) * 128] = (x * gms[b : b + 1, :]).astype(BF16)
    inverse = lax.rsqrt(jnp.sum(square, axis=1, keepdims=True) * (1.0 / WIDTH) + eps)
    acc = nt(scaled[...], wall[...]) * inverse
    lanes = iota((ROWS, 128), 1)
    low = lanes < 64
    qk = acc[:, 0:128] * jnp.where(low, 1.0, HDIM ** (-0.5))
    qkb[tp] = qk.astype(BF16)
    start_all(send_qk)
    ns = nso[...]
    dot_n = jnp.sum(jnp.where(low, qk * ns, 0.0), axis=1, keepdims=True)
    dot_k = jnp.sum(jnp.where(low, qk * pltpu.roll(qk, 64, 1), 0.0), axis=1, keepdims=True)
    sm[0:64] = jnp.where(lanes == 0, dot_n, jnp.where(lanes == 1, dot_k, 0.0))
    pb[tp] = jnp.transpose(sm[...])[0:8]
    start_all(send_pb)

    vo = acc[:, 128:256]
    values = jnp.where(low, vo, pltpu.roll(vo, 64, 1))
    outgate = jnp.where(low, pltpu.roll(vo, 64, 1), vo)
    opened = jax.nn.sigmoid(outgate)
    ga = acc[:, 256:384]
    ingate = ga[:, 0:4]
    pre = pltpu.roll(ga, 124, 1)[:, 0:4] + bias[...]
    logforget = -(jnp.maximum(-pre, 0.0) + jnp.log1p(jnp.exp(-jnp.abs(pre))))
    carried = logforget + cols[:, 0:4]
    max_next = jnp.maximum(carried, ingate)
    decay = jnp.exp(carried - max_next)
    inflow = jnp.exp(ingate - max_next)
    floor = jnp.exp(-max_next)
    max_out[...] = max_next
    dec_out[...] = decay
    inf_out[...] = inflow
    vout[...] = values
    head = (lanes >> 4) & 3

    def spread(columns):
        out = jnp.broadcast_to(columns[0], (ROWS, 128))
        for h in range(1, HEADS):
            out = jnp.where(head == h, columns[h], out)
        return out

    def by_head(a):
        return [a[:, h : h + 1] for h in range(HEADS)]

    arrived(1, lambda p: qkb.at[p], tp, tp_pos)
    numerator = jnp.zeros((ROWS, 128), F32)
    own = (lanes >> 4) == (iota((ROWS, 128), 0) & 7)
    for h in range(HEADS):
        q_parts = []
        for s in range(2):
            a, b = qkb[4 * h + 2 * s].astype(F32), qkb[4 * h + 2 * s + 1].astype(F32)
            q_parts.append(jnp.where(low, a, pltpu.roll(b, 64, 1)).astype(BF16))
            kfull[:, h * 256 + s * 128 : h * 256 + (s + 1) * 128] = jnp.where(low, pltpu.roll(a, 64, 1), b).astype(BF16)
        q = jnp.concatenate(q_parts, axis=1)
        pieces = []
        for t in range(4):
            r = nt(q[t * 16 : (t + 1) * 16], memb[h, t * 256 : (t + 1) * 256])
            pieces += [r[0:8, 0:128], r[8:16, 128:256]]
        diagonal = jnp.where(own, jnp.concatenate(pieces, axis=0), 0.0)
        for shift in (64, 32, 16):
            diagonal = diagonal + pltpu.roll(diagonal, shift, 1)
        numerator = jnp.where(head == h, diagonal, numerator)
    arrived(2, lambda p: pb.at[p], tp, tp_pos)
    for h in range(HEADS):
        sm[h * 8 : (h + 1) * 8] = (pb[4 * h] + pb[4 * h + 1]) + (pb[4 * h + 2] + pb[4 * h + 3])
    sums = jnp.transpose(sm[...])[0:ROWS]
    with_n = spread([sums[:, 8 * h : 8 * h + 1] for h in range(HEADS)])
    with_k = spread([sums[:, 8 * h + 1 : 8 * h + 2] for h in range(HEADS)])
    decay_l, inflow_l, floor_l = spread(by_head(decay)), spread(by_head(inflow)), spread(by_head(floor))
    denominator = jnp.maximum(jnp.abs(decay_l * with_n + inflow_l * with_k), floor_l)
    recall = (decay_l * numerator + inflow_l * values * with_k) / denominator
    gated = opened * recall
    gb[tp] = jnp.where(low[0:32], gated[0:32], gated[32:64]).astype(BF16)
    start_all(send_g)

    for c in loads[14:]:
        c.wait()
    arrived(3, lambda p: gb.at[p], tp, tp_pos)
    tops, ends = [], []
    low32 = low[0:32]
    for s in range(8):
        a, b = gb[2 * s].astype(F32), gb[2 * s + 1].astype(F32)
        tops.append(jnp.where(low32, a, pltpu.roll(b, 64, 1)).astype(BF16))
        ends.append(jnp.where(low32, pltpu.roll(a, 64, 1), b).astype(BF16))
    heads = jnp.concatenate([jnp.concatenate(tops, axis=1), jnp.concatenate(ends, axis=1)], axis=0)
    square = jnp.zeros((ROWS, 128), F32)
    for n in range(4):
        part = nn(heads, mixw[:, :, :, n * 512 : (n + 1) * 512].reshape(1024, 512))
        for b in range(4):
            m = (xg[4 * n + b].astype(F32) + part[:, b * 128 : (b + 1) * 128]).astype(BF16)
            mid[4 * n + b] = m
            m = m.astype(F32)
            square += m * m
    inverse = lax.rsqrt(jnp.sum(square, axis=1, keepdims=True) * (1.0 / WIDTH) + eps)
    for b in range(NTP):
        nst[(b // 4) * 64 : (b // 4 + 1) * 64, (b % 4) * 128 : (b % 4 + 1) * 128] = (
            mid[b].astype(F32) * inverse * ges[b : b + 1, :]
        ).astype(BF16)
    sbuf[...] = nn(pbt[...], nst[...]).astype(BF16).reshape(NEP, 16, 512)
    start_all(send_rows)
    rbuf[ep] = sbuf[ep]

    arrived(4, lambda p: rbuf.at[p], ep, ep_pos)
    rows = nn(perm[...], rbuf[...].reshape(256, 512)).astype(BF16)
    gate = jnp.zeros((ROWS, 256), F32)
    up = jnp.zeros((ROWS, 256), F32)
    for q in range(4):
        r = rows[q * 64 : (q + 1) * 64]
        gate += nn(r, egv[0, q * 512 : (q + 1) * 512, :])
        up += nn(r, euv[0, q * 512 : (q + 1) * 512, :])
    hidden = (gate * jax.nn.sigmoid(gate) * up).astype(BF16)
    for n in range(4):
        part = nn(hidden, edv[0, :, n * 512 : (n + 1) * 512]).astype(BF16)
        for b in range(4):
            dbuf[4 * n + b] = part[:, b * 128 : (b + 1) * 128]
    start_all(send_z)
    zbuf[tp] = dbuf[tp]
    arrived(5, lambda p: zbuf.at[p], tp, tp_pos)
    obuf[...] = nn(perm2[...], zbuf[...].reshape(1024, 128)).astype(BF16).reshape(NEP, 16, 128)
    start_all(send_f)
    fbuf[ep] = obuf[ep]
    arrived(6, lambda p: fbuf.at[p], ep, ep_pos)
    both = nn(comb[...], fbuf[...].reshape(256, 128))
    mixed[...] = (mid[tp].astype(F32) + (both[0:64] + both[64:128])).astype(BF16)
    for copy in (send_tok, send_qk, send_pb, send_g, send_rows, send_z, send_f):
        sent_all(copy)


def local(
    tokens, mixer_gain, expert_gain, query_weight, key_weight, value_weight, outgate_weight, ingate_weight,
    forget_weight, forget_bias, mixout_weight, memory_state, norm_state, max_state, expert_gate, expert_up,
    expert_down, routes, route_weights,
):
    hbm = pl.BlockSpec(memory_space=pl.ANY)
    vm = pl.BlockSpec(memory_space=pltpu.VMEM)
    scratch = [
        pltpu.VMEM((NTP, ROWS, 128), BF16),
        pltpu.VMEM((384, WIDTH), BF16),
        pltpu.VMEM((4, WIDTH), BF16), pltpu.VMEM((4, WIDTH), BF16),
        pltpu.VMEM((16, WIDTH), F32),
        pltpu.VMEM((16, 128), F32), pltpu.VMEM((16, 128), F32),
        pltpu.VMEM((ROWS, HEADS, 16, HDIM), F32),
        pltpu.VMEM((HEADS, 1024, HDIM), BF16),
        pltpu.VMEM((ROWS, HEADS, HDIM), F32),
        pltpu.VMEM((NTP, HEADS, 16, WIDTH), BF16),
        pltpu.VMEM((1, WIDTH, 256), BF16), pltpu.VMEM((1, WIDTH, 256), BF16), pltpu.VMEM((1, 256, WIDTH), BF16),
        pltpu.VMEM((128, 128), F32),
        pltpu.VMEM((4, 64), F32), pltpu.VMEM((2, 64), jnp.int32), pltpu.VMEM((2, 64), F32),
        pltpu.VMEM((256, 256), BF16), pltpu.VMEM((256, 1024), BF16),
        pltpu.VMEM((128, 256), BF16), pltpu.VMEM((256, 256), BF16), pltpu.VMEM((256, 256), F32),
        pltpu.VMEM((ROWS, 128), F32),
        pltpu.VMEM((ROWS, WIDTH), BF16),
        pltpu.VMEM((NTP, ROWS, 128), BF16), pltpu.VMEM((NTP, 8, 128), F32),
        pltpu.VMEM((NTP, 32, 128), BF16),
        pltpu.VMEM((NTP, ROWS, 128), BF16), pltpu.VMEM((256, 512), BF16),
        pltpu.VMEM((NEP, 16, 512), BF16), pltpu.VMEM((NEP, 16, 512), BF16),
        pltpu.VMEM((NTP, ROWS, 128), BF16), pltpu.VMEM((NTP, ROWS, 128), BF16),
        pltpu.VMEM((NEP, 16, 128), BF16), pltpu.VMEM((NEP, 16, 128), BF16),
        pltpu.SemaphoreType.DMA((21,)), pltpu.SemaphoreType.DMA((7, 16)), pltpu.SemaphoreType.DMA((7, 16)),
    ]
    mixed, kfull, vals, decay, inflow, max_next = pl.pallas_call(
        body,
        out_shape=[
            jax.ShapeDtypeStruct((ROWS, 128), BF16),
            jax.ShapeDtypeStruct((ROWS, 1024), BF16),
            jax.ShapeDtypeStruct((ROWS, 128), F32),
            jax.ShapeDtypeStruct((ROWS, HEADS), F32),
            jax.ShapeDtypeStruct((ROWS, HEADS), F32),
            jax.ShapeDtypeStruct((ROWS, HEADS), F32),
        ],
        in_specs=[hbm] * 9 + [vm] + [hbm] * 9,
        out_specs=[vm] * 6,
        scratch_shapes=scratch,
        compiler_params=pltpu.CompilerParams(
            collective_id=0, has_side_effects=True, vmem_limit_bytes=40 * 1024 * 1024
        ),
        name="step",
    )(
        tokens, mixer_gain.reshape(16, 128), expert_gain.reshape(16, 128),
        query_weight.T, key_weight.T,
        value_weight.transpose(1, 2, 0).reshape(64, WIDTH), outgate_weight.transpose(1, 2, 0).reshape(64, WIDTH),
        ingate_weight.T, forget_weight.T, forget_bias.reshape(1, HEADS),
        mixout_weight.reshape(HEADS, NTP, 16, WIDTH),
        memory_state, norm_state, max_state.T, expert_gate, expert_up, expert_down, routes.T, route_weights.T,
    )
    keys = kfull.reshape(ROWS, HEADS, HDIM).astype(F32)
    v = vals[:, 0:64].reshape(ROWS, HEADS, 16)
    memory_next = (
        decay[:, :, None, None] * memory_state + (inflow[:, :, None] * v)[:, :, :, None] * keys[:, :, None, :]
    )
    norm_next = decay[:, :, None] * norm_state + inflow[:, :, None] * keys
    return (mixed, memory_next, norm_next, max_next)


def solution(mesh):
    in_specs = (
        P("ep", "tp"), P(), P(), P(None, "tp"), P(None, "tp"), P(None, None, "tp"), P(None, None, "tp"), P(), P(), P(),
        P(), P("ep", None, "tp", None), P("ep", None, None), P("ep", None), P(("ep", "tp"), None, None),
        P(("ep", "tp"), None, None), P(("ep", "tp"), None, None), P("ep", None), P("ep", None),
    )
    out_specs = (P("ep", "tp"), P("ep", None, "tp", None), P("ep", None, None), P("ep", None))
    return jax.shard_map(local, mesh=mesh, in_specs=in_specs, out_specs=out_specs, check_vma=False)
```

```python
import jax
import jax.numpy as jnp
from jax import lax
from jax.experimental import pallas as pl
from jax.experimental.pallas import tpu as pltpu
from jax.sharding import PartitionSpec as P

MESH = pl.DeviceIdType.MESH
F32, BF16 = jnp.float32, jnp.bfloat16
eps = 1e-06
ROWS, WIDTH, NTP, NEP, HEADS, HDIM, CAP, SPLIT = 64, 2048, 16, 16, 4, 256, 4, 4


def nt(a, b):
    return lax.dot_general(a, b, (((1,), (1,)), ((), ())), preferred_element_type=F32)


def nn(a, b):
    return jnp.dot(a, b, preferred_element_type=F32)


def iota(shape, dim):
    return lax.broadcasted_iota(jnp.int32, shape, dim)


FAR_EP = sorted(((dy, dx) for dy in range(4) for dx in range(4) if dy or dx), key=lambda p: (-(min(p[0], 4 - p[0]) + min(p[1], 4 - p[1])), p))
FAR_Z = (4, 3, 5, 2, 6, 1, 7)


def body(
    tok, gain_m, gain_e, qw, kw, vw, ow, igw, fgw, bias, mixout, mem, norm, mstate, egate, eup, edown, rt, rw,
    mixed, keys_out, update_out, decay_out, norm_out, max_out,
    xg, wall, igs, fgs, wgf, gms, ges, memv, memb, normv, mixw, egv, euv, edv, sm, mss, rts, rws, perm, perm2,
    comb, pbt, pbf, nso, scaled, qb, kb, pb, gb, mid, nst, sbuf, rbuf, half32, half16, pair, zsend, zbuf, obuf, fbuf,
    keys, upt, det, mxt, mixv,
    lsem, ssem, fsem, rsem, psem, osem,
):
    ep, tp = lax.axis_index("ep"), lax.axis_index("tp")
    group, chip, core = tp // SPLIT, tp // 2, tp % 2
    other = chip * 2 + (1 - core)
    ey, ex = ep // 4, ep % 4

    def local(i, src, dst):
        return pltpu.make_async_copy(src, dst, lsem.at[i])

    loads = [
        local(0, tok, xg.at[tp]),
        local(1, rt, rts), local(2, rw, rws), local(3, mstate, mss),
        local(4, igw, igs), local(5, fgw, fgs), local(6, gain_m, gms), local(7, gain_e, ges),
        local(8, qw, wall.at[0:64]), local(9, kw, wall.at[64:128]),
        local(10, vw, wall.at[128:192]), local(11, ow, wall.at[192:256]),
        local(12, norm, normv), local(13, mem, memv),
    ]
    loads += [local(14 + h, mixout.at[h], mixw.at[:, h]) for h in range(HEADS)]
    loads += [local(18, egate, egv), local(19, eup, euv), local(20, edown, edv)]
    loads[0].start()

    barrier = pltpu.get_barrier_semaphore()

    def along(d):
        return lax.rem(tp + 2 * d, NTP)

    def across(dy, dx):
        return lax.rem(ey + dy, 4) * 4 + lax.rem(ex + dx, 4)

    def greet(who):
        pl.semaphore_signal(barrier, inc=1, device_id=who, device_id_type=MESH)

    for d in FAR_Z:
        greet((ep, along(d)))
    for dy, dx in FAR_EP:
        greet((across(dy, dx), tp))
    greet((ep, other))
    for c in loads[1:]:
        c.start()

    i, j = iota((256, 256), 0), iota((256, 256), 1)
    perm[...] = (j == (((i >> 2) & 15) << 4) + ((i >> 6) << 2) + (i & 3)).astype(F32).astype(BF16)
    i, c = iota((256, 512), 0), iota((256, 512), 1)
    perm2[...] = (
        (((c >> 7) == ((i >> 2) & 3)) & ((c & 63) == ((i >> 4) << 2) + (i & 3))).astype(F32).astype(BF16)
    )

    def remote(src, dst, sent, got, who):
        return pltpu.make_async_remote_copy(
            src_ref=src, dst_ref=dst, send_sem=sent, recv_sem=got, device_id=who, device_id_type=MESH)

    def own_to(phase, buf, peer):
        return remote(buf.at[tp], buf.at[tp], ssem.at[phase, peer], rsem.at[phase, tp], (ep, peer))

    def forward(phase, buf, slot):
        return remote(buf.at[slot], buf.at[slot], fsem.at[phase, slot], rsem.at[phase, slot], (ep, other))

    def got(phase, buf, slot):
        remote(buf.at[slot], buf.at[slot], ssem.at[phase, slot], rsem.at[phase, slot], (ep, slot)).wait_recv()

    def gather_start(phase, buf):
        for d in FAR_Z:
            own_to(phase, buf, along(d)).start()
        own_to(phase, buf, other).start()

    def gather_pass(phase, buf):
        for d in (1, 7, 2, 6, 3, 5, 4):
            got(phase, buf, along(d))
            forward(phase, buf, along(d)).start()

    def gather_end(phase, buf):
        def step(d, _):
            got(phase, buf, lax.rem(other + 2 * d, NTP))
            return 0
        lax.fori_loop(0, 8, step, 0)

    def gather_sent(phase, buf):
        def step(d, _):
            own_to(phase, buf, along(d)).wait_send()
            forward(phase, buf, along(d)).wait_send()
            return 0
        lax.fori_loop(1, 8, step, 0)
        own_to(phase, buf, other).wait_send()

    def ep_copy(phase, src, dst, peer):
        return remote(src.at[peer], dst.at[ep], ssem.at[phase, peer], rsem.at[phase, ep], (peer, tp))

    def ep_start(phase, src, dst):
        for dy, dx in FAR_EP:
            ep_copy(phase, src, dst, across(dy, dx)).start()

    def ep_end(phase, dst):
        def step(d, _):
            peer = lax.rem(ep + d, NEP)
            remote(dst.at[peer], dst.at[peer], ssem.at[phase, peer], rsem.at[phase, peer], (peer, tp)).wait_recv()
            return 0
        lax.fori_loop(1, 16, step, 0)

    def ep_sent(phase, src, dst):
        def step(d, _):
            ep_copy(phase, src, dst, lax.rem(ep + d, NEP)).wait_send()
            return 0
        lax.fori_loop(1, 16, step, 0)

    pl.semaphore_wait(barrier, 23)
    loads[0].wait()
    gather_start(0, xg)

    for c in loads[1:8]:
        c.wait()
    sm[...] = jnp.zeros((128, 128), F32)
    sm[0:4, 0:64] = mss[...]
    sm[4:6, 0:64] = rws[...]
    sm[6:8, 0:64] = rts[...].astype(F32)
    cols = jnp.transpose(sm[...])[0:ROWS]
    w0, w1, r0, r1 = cols[:, 4:5], cols[:, 5:6], cols[:, 6:7], cols[:, 7:8]
    total = w0 + w1
    before = (iota((ROWS, ROWS), 1) < iota((ROWS, ROWS), 0)).astype(F32).astype(BF16)
    lane = iota((ROWS, 256), 1)
    slot_of = (lane & 3).astype(F32)
    expert = (lane >> 2).astype(F32)
    zero = jnp.zeros((ROWS, 256), F32)
    named0, named1 = r0 == expert, r1 == expert
    hit = jnp.where(named0 | named1, 1.0, zero)
    share = jnp.where(named0, w0 / total, zero) + jnp.where(named1, w1 / total, zero)
    share = jnp.where(nn(before, hit.astype(BF16)) == slot_of, share, zero)
    high = share.astype(BF16)
    comb[0:64] = high
    comb[64:128] = (share - high.astype(F32)).astype(BF16)
    expert = ((lane >> 4) * SPLIT + group).astype(F32)
    hit = jnp.where((r0 == expert) | (r1 == expert), 1.0, zero)
    pick = jnp.where(nn(before, hit.astype(BF16)) == slot_of, hit, zero)
    quarter = (lane >> 2) & 3
    for q in range(4):
        pbf[q * 64 : (q + 1) * 64] = jnp.where(quarter == q, pick, zero)
    pbt[...] = jnp.transpose(pbf[...]).astype(BF16)

    wgf[...] = jnp.zeros((16, WIDTH), F32)
    wgf[0:4] = igs[...].astype(F32)
    wgf[4:8] = fgs[...].astype(F32)
    wall[256:384] = jnp.zeros((128, WIDTH), BF16)
    wall[256:272] = wgf[...].astype(BF16)
    for c in loads[8:14]:
        c.wait()

    def narrow(k, _):
        at = pl.multiple_of(k * 8, 8)
        to = pl.multiple_of(k * 128, 128)
        for h in range(HEADS):
            memb[h, pl.ds(to, 128), :] = memv[pl.ds(at, 8), h].reshape(128, HDIM).astype(BF16)
        return 0

    lax.fori_loop(0, 8, narrow, 0)
    place = jnp.full((ROWS, 128), tp, jnp.int32)
    chosen = jnp.zeros((ROWS, 128), F32)
    for half in range(8):
        piece = normv[:, half // 2, (half % 2) * 128 : (half % 2 + 1) * 128]
        chosen = jnp.where(place >> 1 == half, piece, chosen)
    nso[...] = jnp.where((place & 1) == 1, pltpu.roll(chosen, 64, 1), chosen)

    gather_pass(0, xg)
    gather_end(0, xg)
    square = jnp.zeros((ROWS, 128), F32)
    for b in range(NTP):
        x = xg[b].astype(F32)
        square += x * x
        scaled[:, b * 128 : (b + 1) * 128] = (x * gms[b : b + 1, :]).astype(BF16)
    inverse = lax.rsqrt(jnp.sum(square, axis=1, keepdims=True) * (1.0 / WIDTH) + eps)
    acc = nt(scaled[...], wall[...]) * inverse
    lanes = iota((ROWS, 128), 1)
    low = lanes < 64
    low32 = low[0:32]
    qk = acc[:, 0:128] * jnp.where(low, 1.0, HDIM ** (-0.5))
    kq = pltpu.roll(qk, 64, 1)
    qb[tp] = jnp.where(low32, qk[0:32], kq[32:64]).astype(BF16)
    kb[tp] = jnp.where(low32, kq[0:32], qk[32:64]).astype(BF16)
    gather_start(1, qb)
    dot_n = jnp.sum(jnp.where(low, qk * nso[...], 0.0), axis=1, keepdims=True)
    dot_k = jnp.sum(jnp.where(low, qk * kq, 0.0), axis=1, keepdims=True)
    sm[0:64] = jnp.where(lanes == 0, dot_n, 0.0)
    sm[64:128] = jnp.where(lanes == 0, dot_k, 0.0)
    pb[tp] = jnp.transpose(sm[...])[0:1]
    gather_start(2, pb)

    vo = acc[:, 128:256]
    ov = pltpu.roll(vo, 64, 1)
    values = jnp.where(low, vo, ov)
    opened = jax.nn.sigmoid(jnp.where(low, ov, vo))
    ga = acc[:, 256:384]
    ingate = ga[:, 0:4]
    pre = pltpu.roll(ga, 124, 1)[:, 0:4] + bias[...]
    logforget = -(jnp.maximum(-pre, 0.0) + jnp.log1p(jnp.exp(-jnp.abs(pre))))
    carried = logforget + cols[:, 0:4]
    max_next = jnp.maximum(carried, ingate)
    decay = jnp.exp(carried - max_next)
    inflow = jnp.exp(ingate - max_next)
    floor = jnp.exp(-max_next)
    head = (lanes >> 4) & 3

    def spread(columns):
        out = jnp.broadcast_to(columns[0], (ROWS, 128))
        for h in range(1, HEADS):
            out = jnp.where(head == h, columns[h], out)
        return out

    def by_head(a):
        return [a[:, h : h + 1] for h in range(HEADS)]

    decay_l, inflow_l, floor_l = spread(by_head(decay)), spread(by_head(inflow)), spread(by_head(floor))
    pushed = inflow_l * values

    def settle(buf, out, k):
        c = pltpu.make_async_copy(buf, out, osem.at[k])
        c.start()
        return c

    outs = []
    sm[0:64] = pushed
    upt[...] = jnp.transpose(sm[...])[0:64]
    sm[0:64] = decay_l
    det[...] = jnp.transpose(sm[...])[0:64]
    sm[0:64, 0:4] = max_next
    mxt[...] = jnp.transpose(sm[...])[0:4, 0:64]
    outs += [settle(upt, update_out, 0), settle(det, decay_out, 1), settle(mxt, max_out, 2)]
    gather_sent(0, xg)

    def unpacked(buf, s):
        a, b = buf[2 * s].astype(F32), buf[2 * s + 1].astype(F32)
        top = jnp.where(low32, a, pltpu.roll(b, 64, 1))
        end = jnp.where(low32, pltpu.roll(a, 64, 1), b)
        return jnp.concatenate([top, end], axis=0)

    gather_pass(1, qb)
    gather_pass(2, pb)
    gather_end(1, qb)
    numerator = jnp.zeros((ROWS, 128), F32)
    mine = (lanes >> 4) == (iota((ROWS, 128), 0) & 7)
    for h in range(HEADS):
        q = jnp.concatenate([unpacked(qb, 2 * h), unpacked(qb, 2 * h + 1)], axis=1).astype(BF16)
        pieces = []
        for t in range(4):
            r = nt(q[t * 16 : (t + 1) * 16], memb[h, t * 256 : (t + 1) * 256])
            pieces += [r[0:8, 0:128], r[8:16, 128:256]]
        diagonal = jnp.where(mine, jnp.concatenate(pieces, axis=0), 0.0)
        for shift in (64, 32, 16):
            diagonal = diagonal + pltpu.roll(diagonal, shift, 1)
        numerator = jnp.where(head == h, diagonal, numerator)
    gather_end(2, pb)
    for h in range(HEADS):
        sm[h : h + 1] = (pb[4 * h] + pb[4 * h + 1]) + (pb[4 * h + 2] + pb[4 * h + 3])
    sums = jnp.transpose(sm[...])
    with_n = spread(by_head(sums[0:64]))
    with_k = spread(by_head(sums[64:128]))
    denominator = jnp.maximum(jnp.abs(decay_l * with_n + inflow_l * with_k), floor_l)
    gated = opened * ((decay_l * numerator + pushed * with_k) / denominator)
    gb[tp] = jnp.where(low32, gated[0:32], gated[32:64]).astype(BF16)
    gather_start(3, gb)
    gather_start(4, kb)

    for c in loads[14:]:
        c.wait()
    gather_sent(1, qb)
    gather_sent(2, pb)
    gather_pass(3, gb)
    gather_end(3, gb)
    heads = jnp.concatenate([unpacked(gb, s) for s in range(8)], axis=1).astype(BF16)
    square = jnp.zeros((ROWS, 128), F32)
    for n in range(4):
        part = nn(heads, mixw[:, :, :, n * 512 : (n + 1) * 512].reshape(1024, 512))
        for b in range(4):
            m = (xg[4 * n + b].astype(F32) + part[:, b * 128 : (b + 1) * 128]).astype(BF16)
            mid[4 * n + b] = m
            m = m.astype(F32)
            square += m * m
    inverse = lax.rsqrt(jnp.sum(square, axis=1, keepdims=True) * (1.0 / WIDTH) + eps)
    for b in range(NTP):
        nst[(b // 4) * 64 : (b // 4 + 1) * 64, (b % 4) * 128 : (b % 4 + 1) * 128] = (
            mid[b].astype(F32) * inverse * ges[b : b + 1, :]
        ).astype(BF16)
    sbuf[...] = nn(pbt[...], nst[...]).astype(BF16).reshape(NEP, 16, 512)
    ep_start(5, sbuf, rbuf)
    rbuf[ep] = sbuf[ep]

    gather_pass(4, kb)
    gather_sent(3, gb)
    gather_end(4, kb)
    for h in range(HEADS):
        k = jnp.concatenate([unpacked(kb, 2 * h), unpacked(kb, 2 * h + 1)], axis=1)
        keys[:, h, :] = k
        normv[:, h, :] = decay[:, h : h + 1] * normv[:, h, :] + inflow[:, h : h + 1] * k
    outs += [settle(keys, keys_out, 3), settle(normv, norm_out, 4)]

    ep_end(5, rbuf)
    rows = nn(perm[...], rbuf[...].reshape(256, 512)).astype(BF16)
    gate = jnp.zeros((ROWS, 256), F32)
    up = jnp.zeros((ROWS, 256), F32)
    for q in range(4):
        r = rows[q * 64 : (q + 1) * 64]
        gate += nn(r, egv[0, q * 512 : (q + 1) * 512, :])
        up += nn(r, euv[0, q * 512 : (q + 1) * 512, :])
    hidden = (gate * jax.nn.sigmoid(gate) * up).astype(BF16)
    for n in range(4):
        part = nn(hidden, edv[0, :, n * 512 : (n + 1) * 512])
        for b in range(4):
            piece = part[:, b * 128 : (b + 1) * 128]
            half32[b % 2, 2 * n + b // 2] = piece
            half16[b % 2, 2 * n + b // 2] = piece.astype(BF16)

    def to_other(z):
        return remote(half16.at[1 - core, z], pair.at[z], psem.at[0, z], psem.at[1, z], (ep, other))

    def to_owner(z):
        return remote(zsend.at[z], zbuf.at[chip], ssem.at[6, z], rsem.at[6, chip], (ep, 2 * z + core))

    def ahead(d):
        return lax.rem(chip + d, 8)

    for d in FAR_Z + (0,):
        to_other(ahead(d)).start()
    for d in FAR_Z:
        z = ahead(d)
        to_other(z).wait_recv()
        zsend[z] = (half32[core, z] + pair[z].astype(F32)).astype(BF16)
        to_owner(z).start()
    to_other(chip).wait_recv()
    zbuf[chip] = (half32[core, chip] + pair[chip].astype(F32)).astype(BF16)
    gather_sent(4, kb)
    ep_sent(5, sbuf, rbuf)

    def landed(d, _):
        z = ahead(d)
        remote(zbuf.at[z], zbuf.at[z], ssem.at[6, z], rsem.at[6, z], (ep, 2 * z + core)).wait_recv()
        return 0

    lax.fori_loop(1, 8, landed, 0)
    obuf[...] = nn(perm2[...], zbuf[...].reshape(512, 128)).astype(BF16).reshape(NEP, 16, 128)
    ep_start(7, obuf, fbuf)
    fbuf[ep] = obuf[ep]

    def left(d, _):
        to_other(ahead(d)).wait_send()
        return 0

    lax.fori_loop(0, 8, left, 0)

    def gone(d, _):
        to_owner(ahead(d)).wait_send()
        return 0

    lax.fori_loop(1, 8, gone, 0)
    for c in outs:
        c.wait()
    ep_end(7, fbuf)
    both = nn(comb[...], fbuf[...].reshape(256, 128))
    mixv[...] = (mid[tp].astype(F32) + (both[0:64] + both[64:128])).astype(BF16)
    last = settle(mixv, mixed, 5)
    ep_sent(7, obuf, fbuf)
    last.wait()


STEP = 8


def finish(mem, keys, update, decay, norm, maxt, mixed, memory_next, norm_next, max_next, mixed_next):
    at = lax.rem(128 - pl.program_id(0) * STEP, 128)
    u = pltpu.roll(update[...], at, 1)
    d = pltpu.roll(decay[...], at, 1)
    for b in range(STEP):
        for h in range(HEADS):
            uc = u[h * 16 : (h + 1) * 16, b : b + 1]
            dc = d[h * 16 : (h + 1) * 16, b : b + 1]
            memory_next[b, h] = dc * mem[b, h] + uc * keys[b, h : h + 1, :]
    norm_next[...] = norm[...]
    max_next[...] = maxt[...]
    mixed_next[...] = mixed[...]


def local(
    tokens, mixer_gain, expert_gain, query_weight, key_weight, value_weight, outgate_weight, ingate_weight,
    forget_weight, forget_bias, mixout_weight, memory_state, norm_state, max_state, expert_gate, expert_up,
    expert_down, routes, route_weights,
):
    hbm = pl.BlockSpec(memory_space=pl.ANY)
    vm = pl.BlockSpec(memory_space=pltpu.VMEM)
    v, dma = pltpu.VMEM, pltpu.SemaphoreType.DMA
    scratch = [
        v((NTP, ROWS, 128), BF16),
        v((384, WIDTH), BF16),
        v((4, WIDTH), BF16), v((4, WIDTH), BF16),
        v((16, WIDTH), F32),
        v((16, 128), F32), v((16, 128), F32),
        v((ROWS, HEADS, 16, HDIM), F32),
        v((HEADS, 1024, HDIM), BF16),
        v((ROWS, HEADS, HDIM), F32),
        v((NTP, HEADS, 16, WIDTH), BF16),
        v((1, WIDTH, 256), BF16), v((1, WIDTH, 256), BF16), v((1, 256, WIDTH), BF16),
        v((128, 128), F32),
        v((4, 64), F32), v((2, 64), jnp.int32), v((2, 64), F32),
        v((256, 256), BF16), v((256, 512), BF16),
        v((128, 256), BF16), v((256, 256), BF16), v((256, 256), F32),
        v((ROWS, 128), F32),
        v((ROWS, WIDTH), BF16),
        v((NTP, 32, 128), BF16), v((NTP, 32, 128), BF16), v((NTP, 1, 128), F32),
        v((NTP, 32, 128), BF16),
        v((NTP, ROWS, 128), BF16), v((256, 512), BF16),
        v((NEP, 16, 512), BF16), v((NEP, 16, 512), BF16),
        v((2, 8, ROWS, 128), F32), v((2, 8, ROWS, 128), BF16),
        v((8, ROWS, 128), BF16), v((8, ROWS, 128), BF16), v((8, ROWS, 128), BF16),
        v((NEP, 16, 128), BF16), v((NEP, 16, 128), BF16),
        v((ROWS, HEADS, HDIM), F32),
        v((64, 128), F32), v((64, 128), F32), v((HEADS, ROWS), F32), v((ROWS, 128), BF16),
        dma((21,)), dma((8, 16)), dma((5, 16)), dma((8, 16)), dma((2, 8)), dma((6,)),
    ]
    shape = jax.ShapeDtypeStruct
    mixed, keys, update, decay, norm_next, max_next = pl.pallas_call(
        body,
        out_shape=[
            shape((ROWS, 128), BF16), shape((ROWS, HEADS, HDIM), F32), shape((64, 128), F32), shape((64, 128), F32),
            shape((ROWS, HEADS, HDIM), F32), shape((HEADS, ROWS), F32),
        ],
        in_specs=[hbm] * 9 + [vm] + [hbm] * 9,
        out_specs=[hbm] * 6,
        scratch_shapes=scratch,
        compiler_params=pltpu.CompilerParams(
            collective_id=0, has_side_effects=True, vmem_limit_bytes=67043328
        ),
        name="step",
    )(
        tokens, mixer_gain.reshape(16, 128), expert_gain.reshape(16, 128),
        query_weight.T, key_weight.T,
        value_weight.transpose(1, 2, 0).reshape(64, WIDTH), outgate_weight.transpose(1, 2, 0).reshape(64, WIDTH),
        ingate_weight.T, forget_weight.T, forget_bias.reshape(1, HEADS),
        mixout_weight.reshape(HEADS, NTP, 16, WIDTH),
        memory_state, norm_state, max_state.T, expert_gate, expert_up, expert_down, routes.T, route_weights.T,
    )

    def rows(*rest):
        return pl.BlockSpec((STEP, *rest), lambda i: (i,) + (0,) * len(rest))

    def whole(*full):
        return pl.BlockSpec(full, lambda i: (0,) * len(full))

    memory_next, norm_next, max_next, mixed = pl.pallas_call(
        finish,
        grid=(ROWS // STEP,),
        out_shape=[
            shape(memory_state.shape, F32), shape((ROWS, HEADS, HDIM), F32), shape((HEADS, ROWS), F32),
            shape((ROWS, 128), BF16),
        ],
        in_specs=[
            rows(HEADS, 16, HDIM), rows(HEADS, HDIM), whole(64, 128), whole(64, 128), rows(HEADS, HDIM),
            whole(HEADS, ROWS), whole(ROWS, 128),
        ],
        out_specs=[rows(HEADS, 16, HDIM), rows(HEADS, HDIM), whole(HEADS, ROWS), whole(ROWS, 128)],
        compiler_params=pltpu.CompilerParams(vmem_limit_bytes=67043328),
        name="finish",
    )(memory_state, keys, update, decay, norm_next, max_next, mixed)
    return (mixed, memory_next, norm_next, max_next.T)


def solution(mesh):
    in_specs = (
        P("ep", "tp"), P(), P(), P(None, "tp"), P(None, "tp"), P(None, None, "tp"), P(None, None, "tp"), P(), P(), P(),
        P(), P("ep", None, "tp", None), P("ep", None, None), P("ep", None), P(("ep", "tp"), None, None),
        P(("ep", "tp"), None, None), P(("ep", "tp"), None, None), P("ep", None), P("ep", None),
    )
    out_specs = (P("ep", "tp"), P("ep", None, "tp", None), P("ep", None, None), P("ep", None))
    return jax.shard_map(local, mesh=mesh, in_specs=in_specs, out_specs=out_specs, check_vma=False)
```

```python
import jax
import jax.numpy as jnp
from jax import lax
from jax.experimental import pallas as pl
from jax.experimental.pallas import tpu as pltpu
from jax.sharding import PartitionSpec as P

MESH = pl.DeviceIdType.MESH
F32, BF16 = jnp.float32, jnp.bfloat16
eps = 1e-06
ROWS, WIDTH, NTP, NEP, HEADS, HDIM, CAP, SPLIT = 64, 2048, 16, 16, 4, 256, 4, 4


def nt(a, b):
    return lax.dot_general(a, b, (((1,), (1,)), ((), ())), preferred_element_type=F32)


def nn(a, b):
    return jnp.dot(a, b, preferred_element_type=F32)


def iota(shape, dim):
    return lax.broadcasted_iota(jnp.int32, shape, dim)


FAR_EP = sorted(((dy, dx) for dy in range(4) for dx in range(4) if dy or dx), key=lambda p: (-(min(p[0], 4 - p[0]) + min(p[1], 4 - p[1])), p))
FAR_Z = (4, 3, 5, 2, 6, 1, 7)
DIRECT = (1, 2, 3)


STEP = 8


def body(
    tok, gain_m, gain_e, qw, kw, vw, ow, igw, fgw, bias, mixout, mem, norm, mstate, egate, eup, edown, rt, rw,
    mixed, mem_out, norm_out, max_out,
    xg, wall, igs, fgs, wgf, gms, ges, memv, memb, normv, mixw, egv, euv, edv, sm, mss, rts, rws, perm, perm2,
    comb, pbt, pbf, nso, biasv, scaled, qb, kb, pb, gb, mid, nst, sbuf, rbuf, half32, half16, pair, zsend, zbuf, obuf, fbuf,
    keys, upt, det, mxt, mixv,
    lsem, ssem, fsem, rsem, psem, osem,
):
    ep, tp = lax.axis_index("ep"), lax.axis_index("tp")
    group, chip, core = tp // SPLIT, tp // 2, tp % 2
    other = chip * 2 + (1 - core)
    opposite = lax.rem(other + 8, NTP)
    ey, ex = ep // 4, ep % 4

    def local(i, src, dst):
        return pltpu.make_async_copy(src, dst, lsem.at[i])

    loads = [
        local(0, tok, xg.at[tp]),
        local(1, rt, rts), local(2, rw, rws), local(3, mstate, mss),
        local(4, igw, igs), local(5, fgw, fgs), local(6, gain_m, gms), local(7, gain_e, ges),
        local(8, qw, wall.at[0:64]), local(9, kw, wall.at[64:128]),
        local(10, vw, wall.at[128:192]), local(11, ow, wall.at[192:256]),
        local(12, norm, normv), local(13, mem, memv),
    ]
    loads += [local(14 + h, mixout.at[h], mixw.at[:, h]) for h in range(HEADS)]
    loads += [local(21, bias, biasv)]
    loads += [local(18, egate, egv), local(19, eup, euv), local(20, edown, edv)]
    loads[0].start()

    barrier = pltpu.get_barrier_semaphore()

    def along(d):
        return lax.rem(tp + 2 * d, NTP)

    def across(dy, dx):
        return lax.rem(ey + dy, 4) * 4 + lax.rem(ex + dx, 4)

    def greet(who):
        pl.semaphore_signal(barrier, inc=1, device_id=who, device_id_type=MESH)

    for d in FAR_Z:
        greet((ep, along(d)))
    for dy, dx in FAR_EP:
        greet((across(dy, dx), tp))
    greet((ep, other))
    greet((ep, opposite))
    for c in loads[1:]:
        c.start()

    i, j = iota((256, 256), 0), iota((256, 256), 1)
    perm[...] = (j == (((i >> 2) & 15) << 4) + ((i >> 6) << 2) + (i & 3)).astype(F32).astype(BF16)
    i, c = iota((256, 512), 0), iota((256, 512), 1)
    perm2[...] = (
        (((c >> 7) == ((i >> 2) & 3)) & ((c & 63) == ((i >> 4) << 2) + (i & 3))).astype(F32).astype(BF16)
    )

    def remote(src, dst, sent, got, who):
        return pltpu.make_async_remote_copy(
            src_ref=src, dst_ref=dst, send_sem=sent, recv_sem=got, device_id=who, device_id_type=MESH)

    def own_to(phase, buf, peer):
        return remote(buf.at[tp], buf.at[tp], ssem.at[phase, peer], rsem.at[phase, tp], (ep, peer))

    def forward(phase, buf, slot):
        return remote(buf.at[slot], buf.at[slot], fsem.at[phase, slot], rsem.at[phase, slot], (ep, other))

    def got(phase, buf, slot):
        remote(buf.at[slot], buf.at[slot], ssem.at[phase, slot], rsem.at[phase, slot], (ep, slot)).wait_recv()

    def gather_start(phase, buf):
        for d in FAR_Z:
            own_to(phase, buf, along(d)).start()
            if d == 4 and phase in DIRECT:
                own_to(phase, buf, opposite).start()
        own_to(phase, buf, other).start()

    def gather_pass(phase, buf):
        for d in (1, 7, 2, 6, 3, 5) if phase in DIRECT else (1, 7, 2, 6, 3, 5, 4):
            got(phase, buf, along(d))
            forward(phase, buf, along(d)).start()

    def gather_end(phase, buf):
        def step(d, _):
            got(phase, buf, lax.rem(other + 2 * d, NTP))
            return 0
        lax.fori_loop(0, 8, step, 0)
        if phase in DIRECT:
            got(phase, buf, along(4))

    def gather_sent(phase, buf):
        def step(d, _):
            own_to(phase, buf, along(d)).wait_send()
            return 0
        lax.fori_loop(1, 8, step, 0)
        own_to(phase, buf, other).wait_send()
        if phase in DIRECT:
            own_to(phase, buf, opposite).wait_send()
        for d in (1, 7, 2, 6, 3, 5) if phase in DIRECT else (1, 7, 2, 6, 3, 5, 4):
            forward(phase, buf, along(d)).wait_send()

    def ep_copy(phase, src, dst, peer):
        return remote(src.at[peer], dst.at[ep], ssem.at[phase, peer], rsem.at[phase, ep], (peer, tp))

    def ep_start(phase, src, dst):
        for dy, dx in FAR_EP:
            ep_copy(phase, src, dst, across(dy, dx)).start()

    def ep_end(phase, dst):
        def step(d, _):
            peer = lax.rem(ep + d, NEP)
            remote(dst.at[peer], dst.at[peer], ssem.at[phase, peer], rsem.at[phase, peer], (peer, tp)).wait_recv()
            return 0
        lax.fori_loop(1, 16, step, 0)

    def ep_sent(phase, src, dst):
        def step(d, _):
            ep_copy(phase, src, dst, lax.rem(ep + d, NEP)).wait_send()
            return 0
        lax.fori_loop(1, 16, step, 0)

    pl.semaphore_wait(barrier, 24)
    loads[0].wait()
    gather_start(0, xg)

    for c in loads[1:8] + loads[18:19]:
        c.wait()
    sm[...] = jnp.zeros((128, 128), F32)
    sm[0:4, 0:64] = mss[...]
    sm[4:6, 0:64] = rws[...]
    sm[6:8, 0:64] = rts[...].astype(F32)
    cols = jnp.transpose(sm[...])[0:ROWS]
    w0, w1, r0, r1 = cols[:, 4:5], cols[:, 5:6], cols[:, 6:7], cols[:, 7:8]
    total = w0 + w1
    before = (iota((ROWS, ROWS), 1) < iota((ROWS, ROWS), 0)).astype(F32).astype(BF16)
    lane = iota((ROWS, 256), 1)
    slot_of = (lane & 3).astype(F32)
    expert = (lane >> 2).astype(F32)
    zero = jnp.zeros((ROWS, 256), F32)
    named0, named1 = r0 == expert, r1 == expert
    hit = jnp.where(named0 | named1, 1.0, zero)
    share = jnp.where(named0, w0 / total, zero) + jnp.where(named1, w1 / total, zero)
    share = jnp.where(nn(before, hit.astype(BF16)) == slot_of, share, zero)
    high = share.astype(BF16)
    comb[0:64] = high
    comb[64:128] = (share - high.astype(F32)).astype(BF16)
    expert = ((lane >> 4) * SPLIT + group).astype(F32)
    hit = jnp.where((r0 == expert) | (r1 == expert), 1.0, zero)
    pick = jnp.where(nn(before, hit.astype(BF16)) == slot_of, hit, zero)
    quarter = (lane >> 2) & 3
    for q in range(4):
        pbf[q * 64 : (q + 1) * 64] = jnp.where(quarter == q, pick, zero)
    pbt[...] = jnp.transpose(pbf[...]).astype(BF16)

    wgf[...] = jnp.zeros((16, WIDTH), F32)
    wgf[0:4] = igs[...].astype(F32)
    wgf[4:8] = fgs[...].astype(F32)
    wall[256:384] = jnp.zeros((128, WIDTH), BF16)
    wall[256:272] = wgf[...].astype(BF16)
    for c in loads[8:14]:
        c.wait()

    def narrow(k, _):
        at = pl.multiple_of(k * 8, 8)
        to = pl.multiple_of(k * 128, 128)
        for h in range(HEADS):
            memb[h, pl.ds(to, 128), :] = memv[pl.ds(at, 8), h].reshape(128, HDIM).astype(BF16)
        return 0

    lax.fori_loop(0, 8, narrow, 0)
    place = jnp.full((ROWS, 128), tp, jnp.int32)
    chosen = jnp.zeros((ROWS, 128), F32)
    for half in range(8):
        piece = normv[:, half // 2, (half % 2) * 128 : (half % 2 + 1) * 128]
        chosen = jnp.where(place >> 1 == half, piece, chosen)
    nso[...] = jnp.where((place & 1) == 1, pltpu.roll(chosen, 64, 1), chosen)

    gather_pass(0, xg)
    gather_end(0, xg)
    square = jnp.zeros((ROWS, 128), F32)
    for b in range(NTP):
        x = xg[b].astype(F32)
        square += x * x
        scaled[:, b * 128 : (b + 1) * 128] = (x * gms[b : b + 1, :]).astype(BF16)
    inverse = lax.rsqrt(jnp.sum(square, axis=1, keepdims=True) * (1.0 / WIDTH) + eps)
    acc = nt(scaled[...], wall[...]) * inverse
    lanes = iota((ROWS, 128), 1)
    low = lanes < 64
    low32 = low[0:32]
    qk = acc[:, 0:128] * jnp.where(low, 1.0, HDIM ** (-0.5))
    kq = pltpu.roll(qk, 64, 1)
    qb[tp] = jnp.where(low32, qk[0:32], kq[32:64]).astype(BF16)
    kb[tp] = jnp.where(low32, kq[0:32], qk[32:64]).astype(BF16)
    gather_start(1, qb)
    dot_n = jnp.sum(jnp.where(low, qk * nso[...], 0.0), axis=1, keepdims=True)
    dot_k = jnp.sum(jnp.where(low, qk * kq, 0.0), axis=1, keepdims=True)
    sm[0:64] = jnp.where(lanes == 0, dot_n, 0.0)
    sm[64:128] = jnp.where(lanes == 0, dot_k, 0.0)
    pb[tp] = jnp.transpose(sm[...])[0:1]
    gather_start(2, pb)

    vo = acc[:, 128:256]
    ov = pltpu.roll(vo, 64, 1)
    values = jnp.where(low, vo, ov)
    opened = jax.nn.sigmoid(jnp.where(low, ov, vo))
    ga = acc[:, 256:384]
    ingate = ga[:, 0:4]
    pre = pltpu.roll(ga, 124, 1)[:, 0:4] + biasv[...]
    logforget = -(jnp.maximum(-pre, 0.0) + jnp.log1p(jnp.exp(-jnp.abs(pre))))
    carried = logforget + cols[:, 0:4]
    max_next = jnp.maximum(carried, ingate)
    decay = jnp.exp(carried - max_next)
    inflow = jnp.exp(ingate - max_next)
    floor = jnp.exp(-max_next)
    head = (lanes >> 4) & 3

    def spread(columns):
        out = jnp.broadcast_to(columns[0], (ROWS, 128))
        for h in range(1, HEADS):
            out = jnp.where(head == h, columns[h], out)
        return out

    def by_head(a):
        return [a[:, h : h + 1] for h in range(HEADS)]

    decay_l, inflow_l, floor_l = spread(by_head(decay)), spread(by_head(inflow)), spread(by_head(floor))
    pushed = inflow_l * values

    def settle(buf, out, k):
        c = pltpu.make_async_copy(buf, out, osem.at[k])
        c.start()
        return c

    outs = []
    sm[0:64] = pushed
    upt[...] = jnp.transpose(sm[...])[0:64]
    sm[0:64] = decay_l
    det[...] = jnp.transpose(sm[...])[0:64]
    sm[0:64, 0:4] = max_next
    mxt[...] = jnp.transpose(sm[...])[0:4, 0:64]
    outs += [settle(mxt, max_out, 0)]
    gather_sent(0, xg)

    def unpacked(buf, s):
        a, b = buf[2 * s].astype(F32), buf[2 * s + 1].astype(F32)
        top = jnp.where(low32, a, pltpu.roll(b, 64, 1))
        end = jnp.where(low32, pltpu.roll(a, 64, 1), b)
        return jnp.concatenate([top, end], axis=0)

    gather_pass(1, qb)
    gather_pass(2, pb)
    gather_start(4, kb)
    gather_end(1, qb)
    numerator = jnp.zeros((ROWS, 128), F32)
    mine = (lanes >> 4) == (iota((ROWS, 128), 0) & 7)
    for h in range(HEADS):
        q = jnp.concatenate([unpacked(qb, 2 * h), unpacked(qb, 2 * h + 1)], axis=1).astype(BF16)
        pieces = []
        for t in range(4):
            r = nt(q[t * 16 : (t + 1) * 16], memb[h, t * 256 : (t + 1) * 256])
            pieces += [r[0:8, 0:128], r[8:16, 128:256]]
        diagonal = jnp.where(mine, jnp.concatenate(pieces, axis=0), 0.0)
        for shift in (64, 32, 16):
            diagonal = diagonal + pltpu.roll(diagonal, shift, 1)
        numerator = jnp.where(head == h, diagonal, numerator)
    gather_end(2, pb)
    for h in range(HEADS):
        sm[h : h + 1] = (pb[4 * h] + pb[4 * h + 1]) + (pb[4 * h + 2] + pb[4 * h + 3])
    sums = jnp.transpose(sm[...])
    with_n = spread(by_head(sums[0:64]))
    with_k = spread(by_head(sums[64:128]))
    denominator = jnp.maximum(jnp.abs(decay_l * with_n + inflow_l * with_k), floor_l)
    gated = opened * ((decay_l * numerator + pushed * with_k) / denominator)
    gb[tp] = jnp.where(low32, gated[0:32], gated[32:64]).astype(BF16)
    gather_start(3, gb)

    for c in loads[14:18] + loads[19:]:
        c.wait()
    gather_sent(1, qb)
    gather_sent(2, pb)
    gather_pass(3, gb)
    gather_pass(4, kb)
    gather_end(3, gb)
    heads = jnp.concatenate([unpacked(gb, s) for s in range(8)], axis=1).astype(BF16)
    square = jnp.zeros((ROWS, 128), F32)
    for n in range(4):
        part = nn(heads, mixw[:, :, :, n * 512 : (n + 1) * 512].reshape(1024, 512))
        for b in range(4):
            m = (xg[4 * n + b].astype(F32) + part[:, b * 128 : (b + 1) * 128]).astype(BF16)
            mid[4 * n + b] = m
            m = m.astype(F32)
            square += m * m
    inverse = lax.rsqrt(jnp.sum(square, axis=1, keepdims=True) * (1.0 / WIDTH) + eps)
    for b in range(NTP):
        nst[(b // 4) * 64 : (b // 4 + 1) * 64, (b % 4) * 128 : (b % 4 + 1) * 128] = (
            mid[b].astype(F32) * inverse * ges[b : b + 1, :]
        ).astype(BF16)
    sbuf[...] = nn(pbt[...], nst[...]).astype(BF16).reshape(NEP, 16, 512)
    ep_start(5, sbuf, rbuf)
    rbuf[ep] = sbuf[ep]

    gather_sent(3, gb)
    gather_end(4, kb)
    for h in range(HEADS):
        k = jnp.concatenate([unpacked(kb, 2 * h), unpacked(kb, 2 * h + 1)], axis=1)
        keys[:, h, :] = k
        normv[:, h, :] = decay[:, h : h + 1] * normv[:, h, :] + inflow[:, h : h + 1] * k
    outs += [settle(normv, norm_out, 1)]

    def stored(k):
        at = pl.multiple_of(k * STEP, STEP)
        return pltpu.make_async_copy(memv.at[pl.ds(at, STEP)], mem_out.at[pl.ds(at, STEP)], osem.at[5 + k])

    def renew(k, _):
        shift = lax.rem(128 - k * STEP, 128)
        u = pltpu.roll(upt[...], shift, 1)
        d = pltpu.roll(det[...], shift, 1)
        for b in range(STEP):
            for h in range(HEADS):
                uc = u[h * 16 : (h + 1) * 16, b : b + 1]
                dc = d[h * 16 : (h + 1) * 16, b : b + 1]
                memv[k * STEP + b, h] = dc * memv[k * STEP + b, h] + uc * keys[k * STEP + b, h : h + 1, :]
        stored(k).start()
        return 0

    lax.fori_loop(0, 3, renew, 0)

    ep_end(5, rbuf)
    rows = nn(perm[...], rbuf[...].reshape(256, 512)).astype(BF16)
    gate = jnp.zeros((ROWS, 256), F32)
    up = jnp.zeros((ROWS, 256), F32)
    for q in range(4):
        r = rows[q * 64 : (q + 1) * 64]
        gate += nn(r, egv[0, q * 512 : (q + 1) * 512, :])
        up += nn(r, euv[0, q * 512 : (q + 1) * 512, :])
    hidden = (gate * jax.nn.sigmoid(gate) * up).astype(BF16)
    for n in range(4):
        part = nn(hidden, edv[0, :, n * 512 : (n + 1) * 512])
        for b in range(4):
            piece = part[:, b * 128 : (b + 1) * 128]
            half32[b % 2, 2 * n + b // 2] = piece
            half16[b % 2, 2 * n + b // 2] = piece.astype(BF16)

    def to_other(z):
        return remote(half16.at[1 - core, z], pair.at[z], psem.at[0, z], psem.at[1, z], (ep, other))

    def to_owner(z):
        return remote(zsend.at[z], zbuf.at[chip], ssem.at[6, z], rsem.at[6, chip], (ep, 2 * z + core))

    def ahead(d):
        return lax.rem(chip + d, 8)

    for d in FAR_Z + (0,):
        to_other(ahead(d)).start()
    for d in FAR_Z:
        z = ahead(d)
        to_other(z).wait_recv()
        zsend[z] = (half32[core, z] + pair[z].astype(F32)).astype(BF16)
        to_owner(z).start()
    to_other(chip).wait_recv()
    zbuf[chip] = (half32[core, chip] + pair[chip].astype(F32)).astype(BF16)
    lax.fori_loop(3, 6, renew, 0)
    gather_sent(4, kb)
    ep_sent(5, sbuf, rbuf)

    def landed(d, _):
        z = ahead(d)
        remote(zbuf.at[z], zbuf.at[z], ssem.at[6, z], rsem.at[6, z], (ep, 2 * z + core)).wait_recv()
        return 0

    lax.fori_loop(1, 8, landed, 0)
    obuf[...] = nn(perm2[...], zbuf[...].reshape(512, 128)).astype(BF16).reshape(NEP, 16, 128)
    ep_start(7, obuf, fbuf)
    fbuf[ep] = obuf[ep]

    lax.fori_loop(6, 8, renew, 0)

    def left(d, _):
        to_other(ahead(d)).wait_send()
        return 0

    lax.fori_loop(0, 8, left, 0)

    def gone(d, _):
        to_owner(ahead(d)).wait_send()
        return 0

    lax.fori_loop(1, 8, gone, 0)
    for c in outs:
        c.wait()

    def kept(k, _):
        stored(k).wait()
        return 0

    lax.fori_loop(0, 8, kept, 0)
    ep_end(7, fbuf)
    both = nn(comb[...], fbuf[...].reshape(256, 128))
    mixv[...] = (mid[tp].astype(F32) + (both[0:64] + both[64:128])).astype(BF16)
    last = settle(mixv, mixed, 2)
    ep_sent(7, obuf, fbuf)
    last.wait()


def finish(mem, norm, maxt, mixed, mem_to, norm_to, max_to, mixed_to, held, normv, maxv, mixv, came, went):
    pairs = [(mem.at[pl.ds(k * STEP, STEP)], held.at[pl.ds(k * STEP, STEP)], mem_to.at[pl.ds(k * STEP, STEP)]) for k in range(8)]
    pairs += [(norm, normv, norm_to), (maxt, maxv, max_to), (mixed, mixv, mixed_to)]
    ins = [pltpu.make_async_copy(a, b, came.at[k]) for k, (a, b, _) in enumerate(pairs)]
    outs = [pltpu.make_async_copy(b, c, went.at[k]) for k, (_, b, c) in enumerate(pairs)]
    for c in ins:
        c.start()
    for c, o in zip(ins, outs):
        c.wait()
        o.start()
    for o in outs:
        o.wait()


def local(
    tokens, mixer_gain, expert_gain, query_weight, key_weight, value_weight, outgate_weight, ingate_weight,
    forget_weight, forget_bias, mixout_weight, memory_state, norm_state, max_state, expert_gate, expert_up,
    expert_down, routes, route_weights,
):
    hbm = pl.BlockSpec(memory_space=pl.ANY)
    v, dma = pltpu.VMEM, pltpu.SemaphoreType.DMA
    scratch = [
        v((NTP, ROWS, 128), BF16),
        v((384, WIDTH), BF16),
        v((4, WIDTH), BF16), v((4, WIDTH), BF16),
        v((16, WIDTH), F32),
        v((16, 128), F32), v((16, 128), F32),
        v((ROWS, HEADS, 16, HDIM), F32),
        v((HEADS, 1024, HDIM), BF16),
        v((ROWS, HEADS, HDIM), F32),
        v((NTP, HEADS, 16, WIDTH), BF16),
        v((1, WIDTH, 256), BF16), v((1, WIDTH, 256), BF16), v((1, 256, WIDTH), BF16),
        v((128, 128), F32),
        v((4, 64), F32), v((2, 64), jnp.int32), v((2, 64), F32),
        v((256, 256), BF16), v((256, 512), BF16),
        v((128, 256), BF16), v((256, 256), BF16), v((256, 256), F32),
        v((ROWS, 128), F32), v((1, HEADS), F32),
        v((ROWS, WIDTH), BF16),
        v((NTP, 32, 128), BF16), v((NTP, 32, 128), BF16), v((NTP, 1, 128), F32),
        v((NTP, 32, 128), BF16),
        v((NTP, ROWS, 128), BF16), v((256, 512), BF16),
        v((NEP, 16, 512), BF16), v((NEP, 16, 512), BF16),
        v((2, 8, ROWS, 128), F32), v((2, 8, ROWS, 128), BF16),
        v((8, ROWS, 128), BF16), v((8, ROWS, 128), BF16), v((8, ROWS, 128), BF16),
        v((NEP, 16, 128), BF16), v((NEP, 16, 128), BF16),
        v((ROWS, HEADS, HDIM), F32),
        v((64, 128), F32), v((64, 128), F32), v((HEADS, ROWS), F32), v((ROWS, 128), BF16),
        dma((22,)), dma((8, 16)), dma((5, 16)), dma((8, 16)), dma((2, 8)), dma((13,)),
    ]
    shape = jax.ShapeDtypeStruct
    mixed, memory_next, norm_next, max_next = pl.pallas_call(
        body,
        out_shape=[
            shape((ROWS, 128), BF16), shape(memory_state.shape, F32), shape((ROWS, HEADS, HDIM), F32),
            shape((HEADS, ROWS), F32),
        ],
        in_specs=[hbm] * 19,
        out_specs=[hbm] * 4,
        scratch_shapes=scratch,
        compiler_params=pltpu.CompilerParams(
            collective_id=0, has_side_effects=True, vmem_limit_bytes=67043328
        ),
        name="step",
    )(
        tokens, mixer_gain.reshape(16, 128), expert_gain.reshape(16, 128),
        query_weight.T, key_weight.T,
        value_weight.transpose(1, 2, 0).reshape(64, WIDTH), outgate_weight.transpose(1, 2, 0).reshape(64, WIDTH),
        ingate_weight.T, forget_weight.T, forget_bias.reshape(1, HEADS),
        mixout_weight.reshape(HEADS, NTP, 16, WIDTH),
        memory_state, norm_state, max_state.T, expert_gate, expert_up, expert_down, routes.T, route_weights.T,
    )

    kinds = [((ROWS, HEADS, 16, HDIM), F32), ((ROWS, HEADS, HDIM), F32), ((HEADS, ROWS), F32), ((ROWS, 128), BF16)]
    memory_next, norm_next, max_next, mixed = pl.pallas_call(
        finish,
        out_shape=[shape(*k) for k in kinds],
        in_specs=[hbm] * 4,
        out_specs=[hbm] * 4,
        scratch_shapes=[v(*k) for k in kinds] + [dma((11,)), dma((11,))],
        compiler_params=pltpu.CompilerParams(vmem_limit_bytes=67043328),
        name="finish",
    )(memory_next, norm_next, max_next, mixed)
    return (mixed, memory_next, norm_next, max_next.T)


def solution(mesh):
    in_specs = (
        P("ep", "tp"), P(), P(), P(None, "tp"), P(None, "tp"), P(None, None, "tp"), P(None, None, "tp"), P(), P(), P(),
        P(), P("ep", None, "tp", None), P("ep", None, None), P("ep", None), P(("ep", "tp"), None, None),
        P(("ep", "tp"), None, None), P(("ep", "tp"), None, None), P("ep", None), P("ep", None),
    )
    out_specs = (P("ep", "tp"), P("ep", None, "tp", None), P("ep", None, None), P("ep", None))
    return jax.shard_map(local, mesh=mesh, in_specs=in_specs, out_specs=out_specs, check_vma=False)
```
